32 devices in a mesh: fs: 8 (over z, x), tp: 4 (over y, core).
Axes of the slice: x: 2, y: 2, z: 4, core: 2. Of those that a mesh axis runs over, the one named last changes fastest.
Arguments:
- tokens: bfloat16 [2048, 3072], P('tp', 'fs'), may hold values from -6 to 6
- mix_gain: float32 [2048], replicated, may hold values from 0.1 to 1.9
- mlp_gain: float32 [2048], replicated, may hold values from 0.1 to 1.9
- query_weight: float32 [2048, 1024], P('fs', 'tp'), may hold values from -0.125 to 0.125
- key_weight: float32 [2048, 1024], P('fs', 'tp'), may hold values from -0.125 to 0.125
- value_weight: float32 [2048, 1024], P('fs', 'tp'), may hold values from -0.125 to 0.125
- gate_weight: float32 [2048, 1024], P('fs', 'tp'), may hold values from -0.125 to 0.125
- out_weight: float32 [1024, 2048], P('tp', 'fs'), may hold values from -0.1875 to 0.1875
- up_weight: float32 [2048, 8192], P('fs', 'tp'), may hold values from -0.125 to 0.125
- down_weight: float32 [8192, 2048], P('tp', 'fs'), may hold values from -0.0625 to 0.0625
- query_scale: float32 [1024], P(('tp', 'fs')), may hold values from 0.1 to 1.9
- key_scale: float32 [1024], P(('tp', 'fs')), may hold values from 0.1 to 1.9
- value_scale: float32 [1024], P(('tp', 'fs')), may hold values from 0.1 to 1.9
- gate_scale: float32 [1024], P(('tp', 'fs')), may hold values from 0.1 to 1.9
- out_scale: float32 [2048], P(('tp', 'fs')), may hold values from 0.1 to 1.9
- up_scale: float32 [8192], P(('tp', 'fs')), may hold values from 0.1 to 1.9
- down_scale: float32 [2048], P(('tp', 'fs')), may hold values from 0.1 to 1.9
- forget: float32 [16], P('tp'), as said below
Outputs:
- layer_out: bfloat16 [2048, 3072], P('tp', 'fs')
The draws below stay inside these ranges and needn't reach their ends.
Inputs may be any that keep to these rules, and one draw needn't show every extreme that they name: `forget`: positive rates; each head either forgets within a few tens of positions or keeps a tenth or more over a whole sequence of 384.
All inputs are finite; a program needn't handle non-finite values.
Results may differ from the reference program's by a relative error of at most 0.02.
Values may be sent and summed in bfloat16 or wider, within the bound.
No kernel may reach another device: no remote copies, remote signals or barrier semaphores. Data moves between devices by JAX's collectives and lax.ppermute only.
A program may use at most 64 MiB of HBM per device.

```python
import math
import jax
import jax.numpy as jnp
from jax import lax

D = 2048
HEADS = 16
HEAD_DIM = 64
FF = 8192
LEN = 384
RET_W = 1024
TOKENS = 3072
N_FS = 8
N_TP = 4


def draw_forget(key, part):
    first, second, third = jax.random.split(key, 3)
    fast = jax.random.randint(first, (HEADS,), 0, 16) < 8
    quick = jax.random.uniform(second, (HEADS,), jnp.float32, 1.0 / 50.0, 1.0 / 25.0)
    slow = jnp.exp(jax.random.uniform(third, (HEADS,), jnp.float32, math.log(0.1 / LEN), math.log(2.0 / LEN)))
    return jnp.where(fast, quick, slow).astype(jnp.float32)


def shard_levels(key, dims, cuts, smallest, largest):
    factor_of, own = 1.0, jax.random.fold_in(key, 6)
    for dim, shards_of in cuts:
        draws = jnp.exp(jax.random.uniform(jax.random.fold_in(own, dim), (shards_of,), jnp.float32, smallest / len(cuts), largest / len(cuts)))
        factor_of = factor_of * jnp.repeat(draws, dims[dim] // shards_of).reshape([-1 if axis == dim else 1 for axis in range(len(dims))])
    return factor_of


def centred(rng, extent, deviation, limit, cuts=(), held_as=jnp.bfloat16):
    array = deviation * jax.random.normal(rng, extent, jnp.float32)
    if cuts:
        array = array * shard_levels(rng, extent, cuts, -0.22, 0.18)
    return jnp.clip(array, -limit, limit).astype(held_as)


def setup_inputs(seed: int = 0) -> dict:
    key_list = jax.random.split(jax.random.key(seed), 19)
    tokens = centred(key_list[0], (D, TOKENS), 1.0, 6.0, ((0, 4), (1, 8)))
    mix_gain = jnp.clip(1.0 + 0.18 * jax.random.normal(key_list[1], (D,), jnp.float32), 0.1, 1.9)
    mlp_gain = jnp.clip(1.0 + 0.18 * jax.random.normal(key_list[2], (D,), jnp.float32), 0.1, 1.9)
    query_weight = centred(key_list[3], (D, RET_W), D ** -0.5, 0.125, ((0, 8), (1, 4)), jnp.float32)
    key_weight = centred(key_list[4], (D, RET_W), D ** -0.5, 0.125, ((0, 8), (1, 4)), jnp.float32)
    value_weight = centred(key_list[5], (D, RET_W), D ** -0.5, 0.125, ((0, 8), (1, 4)), jnp.float32)
    gate_weight = centred(key_list[6], (D, RET_W), D ** -0.5, 0.125, ((0, 8), (1, 4)), jnp.float32)
    out_weight = centred(key_list[7], (RET_W, D), RET_W ** -0.5, 0.1875, ((0, 4), (1, 8)), jnp.float32)
    up_weight = centred(key_list[8], (D, FF), D ** -0.5, 0.125, ((0, 8), (1, 4)), jnp.float32)
    down_weight = centred(key_list[9], (FF, D), FF ** -0.5, 0.0625, ((0, 4), (1, 8)), jnp.float32)
    query_scale = jnp.clip(1.0 + 0.18 * jax.random.normal(key_list[10], (RET_W,), jnp.float32), 0.1, 1.9)
    key_scale = jnp.clip(1.0 + 0.18 * jax.random.normal(key_list[11], (RET_W,), jnp.float32), 0.1, 1.9)
    value_scale = jnp.clip(1.0 + 0.18 * jax.random.normal(key_list[12], (RET_W,), jnp.float32), 0.1, 1.9)
    gate_scale = jnp.clip(1.0 + 0.18 * jax.random.normal(key_list[13], (RET_W,), jnp.float32), 0.1, 1.9)
    out_scale = jnp.clip(1.0 + 0.18 * jax.random.normal(key_list[14], (D,), jnp.float32), 0.1, 1.9)
    up_scale = jnp.clip(1.0 + 0.18 * jax.random.normal(key_list[15], (FF,), jnp.float32), 0.1, 1.9)
    down_scale = jnp.clip(1.0 + 0.18 * jax.random.normal(key_list[16], (D,), jnp.float32), 0.1, 1.9)
    forget = draw_forget(jax.random.fold_in(key_list[18], 71), 0)
    return dict(tokens=tokens, mix_gain=mix_gain, mlp_gain=mlp_gain, query_weight=query_weight, key_weight=key_weight, value_weight=value_weight, gate_weight=gate_weight, out_weight=out_weight, up_weight=up_weight, down_weight=down_weight, query_scale=query_scale, key_scale=key_scale, value_scale=value_scale, gate_scale=gate_scale, out_scale=out_scale, up_scale=up_scale, down_scale=down_scale, forget=forget)


def rotary(field, pos):
    half = field.shape[-1] // 2
    inverse = 1.0 / 10000.0 ** jnp.linspace(0.0, 1.0, half, dtype=jnp.float32)
    angle = pos[:, None] * inverse[None, :]
    cosine = jnp.cos(angle)[None, :, None, :]
    sine = jnp.sin(angle)[None, :, None, :]
    paired = field.astype(jnp.float32).reshape(field.shape[:-1] + (half, 2))
    first, second = (paired[..., 0], paired[..., 1])
    turned = jnp.stack([first * cosine - second * sine, first * sine + second * cosine], axis=-1)
    return turned.reshape(field.shape)

def retain(query, key, value, gate, forget):
    batch, length, heads, width = query.shape
    block = 128
    count = length // block
    top = lax.Precision.HIGHEST
    pos = jnp.arange(length, dtype=jnp.float32)
    rot_q = rotary(query, pos)
    rot_k = rotary(key, pos) * width ** (-0.5)
    vals = value.astype(jnp.float32)
    log_decay = -forget.astype(jnp.float32)
    steps = jnp.arange(block, dtype=jnp.float32)
    offset = steps[:, None] - steps[None, :]
    decay_mask = jnp.where(offset >= 0, jnp.exp(log_decay[:, None, None] * jnp.maximum(offset, 0.0)), 0.0)
    q_blocks = rot_q.reshape(batch, count, block, heads, width)
    k_blocks = rot_k.reshape(batch, count, block, heads, width)
    v_blocks = vals.reshape(batch, count, block, heads, width)
    inner = jnp.einsum('bnihd,bnjhd->bnhij', q_blocks, k_blocks, precision=top) * decay_mask
    inner = jnp.einsum('bnhij,bnjhe->bnihe', inner, v_blocks, precision=top)
    tail = jnp.exp(log_decay[:, None] * (block - 1.0 - steps)[None, :])
    update = jnp.einsum('bnjhd,bnjhe,hj->nbhde', k_blocks, v_blocks, tail, precision=top)
    block_decay = jnp.exp(log_decay * block)[None, :, None, None]

    def advance(state, piece):
        return (state * block_decay + piece, state)
    start_state = jnp.zeros((batch, heads, width, width), jnp.float32)
    _, before = lax.scan(advance, start_state, update)
    lead = jnp.exp(log_decay[None, :] * (steps[:, None] + 1.0))
    cross = jnp.einsum('bnihd,nbhde->bnihe', q_blocks, before, precision=top) * lead[None, None, :, :, None]
    total = inner + cross
    total = total * lax.rsqrt(lax.optimization_barrier(jnp.mean(total * total, axis=-1, keepdims=True)) + 0.01)
    total = total.reshape(batch, length, heads, width)
    return jax.nn.silu(gate.astype(jnp.float32)) * total

def norm_rows(rows, gain):
    scale = lax.rsqrt(lax.optimization_barrier(jnp.mean(rows * rows, axis=-1, keepdims=True)) + 1e-06)
    return (rows * scale * gain[None, :]).astype(jnp.bfloat16)

def reference(tokens, mix_gain, mlp_gain, query_weight, key_weight, value_weight, gate_weight, out_weight, up_weight, down_weight, query_scale, key_scale, value_scale, gate_scale, out_scale, up_scale, down_scale, forget):
    stream = tokens.astype(jnp.float32).T
    normed = norm_rows(stream, mix_gain)

    def project(weight, scale):
        product = jnp.dot(normed, weight.astype(jnp.bfloat16), preferred_element_type=jnp.float32)
        return (product * scale[None, :]).astype(jnp.bfloat16)
    shape = (N_FS, LEN, HEADS, HEAD_DIM)
    query = project(query_weight, query_scale).reshape(shape)
    key = project(key_weight, key_scale).reshape(shape)
    value = project(value_weight, value_scale).reshape(shape)
    gate = project(gate_weight, gate_scale).reshape(shape)
    mixed_heads = retain(query, key, value, gate, forget).reshape(TOKENS, RET_W).astype(jnp.bfloat16)
    out_b = out_weight.astype(jnp.bfloat16)
    group = RET_W // N_TP

    def mix_group(carry, index):
        rows = lax.dynamic_slice_in_dim(mixed_heads, index * group, group, 1)
        weight = lax.dynamic_slice_in_dim(out_b, index * group, group, 0)
        part = jnp.dot(rows, weight, preferred_element_type=jnp.float32).astype(jnp.bfloat16)
        part = lax.optimization_barrier(part)
        return (carry + part.astype(jnp.float32), None)
    groups = jnp.arange(N_TP, dtype=jnp.int32)
    mix_total, _ = lax.scan(mix_group, jnp.zeros((TOKENS, D), jnp.float32), groups)
    after_mix = (stream + mix_total * out_scale[None, :]).astype(jnp.bfloat16)
    normed_mlp = norm_rows(after_mix.astype(jnp.float32), mlp_gain)
    units = FF // N_TP

    def mlp_group(carry, index):
        w_up = lax.dynamic_slice_in_dim(up_weight, index * units, units, 1).astype(jnp.bfloat16)
        s_up = lax.dynamic_slice_in_dim(up_scale, index * units, units, 0)
        hidden = jnp.dot(normed_mlp, w_up, preferred_element_type=jnp.float32) * s_up[None, :]
        hidden = jnp.square(jax.nn.relu(hidden)).astype(jnp.bfloat16)
        w_down = lax.dynamic_slice_in_dim(down_weight, index * units, units, 0).astype(jnp.bfloat16)
        part = jnp.dot(hidden, w_down, preferred_element_type=jnp.float32).astype(jnp.bfloat16)
        part = lax.optimization_barrier(part)
        return (carry + part.astype(jnp.float32), None)
    mlp_total, _ = lax.scan(mlp_group, jnp.zeros((TOKENS, D), jnp.float32), groups)
    layer_out = (after_mix.astype(jnp.float32) + mlp_total * down_scale[None, :]).astype(jnp.bfloat16)
    return layer_out.T
```

```python
import jax
import jax.numpy as jnp
from jax import lax
from jax.sharding import PartitionSpec as P

BF = jnp.bfloat16
F32 = jnp.float32
PAIR = 2


def swap(array, axis, bit):
    size = lax.axis_size(axis)
    return lax.ppermute(array, axis, [(i, i ^ bit) for i in range(size)])


def bits_of(axis):
    bit, found = 1, []
    while bit < lax.axis_size(axis):
        found.append(bit)
        bit *= 2
    return found


def spread(chunks, axis, bits):
    for bit in bits:
        chunks = {**chunks, **{k ^ bit: swap(c, axis, bit) for k, c in chunks.items()}}
    return chunks


def place(chunks, axis):
    own = lax.axis_index(axis)
    first = chunks[0]
    rows = first.shape[0]
    whole = jnp.zeros((rows * len(chunks),) + first.shape[1:], first.dtype)
    for k, c in chunks.items():
        whole = lax.dynamic_update_slice_in_dim(whole, c, rows * (own ^ k), 0)
    return whole


def collect(mine, other):
    chunks = {0: mine, PAIR: swap(other, "fs", PAIR)}
    return spread(chunks, "fs", [b for b in reversed(bits_of("fs")) if b != PAIR])


def gather_tokens(rows):
    own = lax.axis_index("tp")
    count, length = rows.shape
    whole = jnp.zeros((count * lax.axis_size("tp"), 2 * length), rows.dtype)
    for s, piece in enumerate((rows, swap(rows, "fs", PAIR))):
        for k, c in spread({0: piece}, "tp", list(reversed(bits_of("tp")))).items():
            whole = lax.dynamic_update_slice(whole, c, (count * (own ^ k), length * s))
    return whole


def reduce_tp(part):
    own = lax.axis_index("tp")
    size = lax.axis_size("tp")
    current = part.reshape((size, part.shape[0] // size, part.shape[1]))
    for bit in bits_of("tp"):
        side = (own // bit) % 2
        halves = current.astype(BF).reshape((current.shape[0] // 2, 2) + current.shape[1:])
        kept = lax.dynamic_index_in_dim(halves, side, 1, keepdims=False)
        sent = lax.dynamic_index_in_dim(halves, 1 - side, 1, keepdims=False)
        current = kept.astype(F32) + swap(sent, "tp", bit).astype(F32)
    return current[0]


def norm_columns(whole, gain):
    values = whole.astype(F32)
    scale = lax.rsqrt(jnp.mean(values * values, axis=0, keepdims=True) + 1e-06)
    return (values * scale * gain[:, None]).astype(BF)


def contract_first(left, right):
    return lax.dot_general(left, right, (((0,), (0,)), ((), ())), preferred_element_type=F32)


def tables(length, width, heads):
    half = width // 2
    pos = jnp.arange(length, dtype=F32)
    inverse = 1.0 / 10000.0 ** jnp.linspace(0.0, 1.0, half, dtype=F32)
    angle = pos[:, None] * jnp.repeat(inverse, 2)[None, :]
    return jnp.cos(angle), jnp.sin(angle)


def retain(query, key, value, gate, forget):
    batch, length, heads, width = query.shape
    top = lax.Precision.HIGHEST
    cosine, sine = tables(length, width, heads)
    cosine, sine = cosine[None, :, None, :], sine[None, :, None, :]
    row = jnp.arange(width)[:, None]
    col = jnp.arange(width)[None, :]
    turn = jnp.where(
        (row ^ 1) == col, jnp.where(col % 2 == 0, -1.0, 1.0), 0.0
    ).astype(BF)

    def rotary(field):
        crossed = jnp.einsum("blhd,de->blhe", field, turn, preferred_element_type=F32)
        return field.astype(F32) * cosine + crossed * sine

    rot_q = rotary(query)
    rot_k = rotary(key) * width ** (-0.5)
    steps = jnp.arange(length, dtype=F32)
    offset = steps[:, None] - steps[None, :]
    decay = jnp.where(
        offset >= 0, jnp.exp(-forget[:, None, None] * jnp.maximum(offset, 0.0)), 0.0
    )
    inner = jnp.einsum("bihd,bjhd->bhij", rot_q, rot_k, precision=top) * decay[None]
    total = jnp.einsum("bhij,bjhe->bihe", inner, value.astype(F32), precision=top)
    total = total * lax.rsqrt(jnp.mean(total * total, axis=-1, keepdims=True) + 0.01)
    return jax.nn.silu(gate.astype(F32)) * total


def on_device(
    tokens,
    mix_gain,
    mlp_gain,
    query_weight,
    key_weight,
    value_weight,
    gate_weight,
    out_weight,
    up_weight,
    down_weight,
    query_scale,
    key_scale,
    value_scale,
    gate_scale,
    out_scale,
    up_scale,
    down_scale,
    forget,
):
    length = tokens.shape[1]
    side = (lax.axis_index("fs") // PAIR) % 2

    def halves(array, dim):
        size = array.shape[dim] // 2
        low = lax.slice_in_dim(array, 0, size, axis=dim)
        high = lax.slice_in_dim(array, size, 2 * size, axis=dim)
        return jnp.where(side == 0, low, high), jnp.where(side == 0, high, low)

    fs_bits = list(reversed(bits_of("fs")))
    whole = gather_tokens(tokens)

    pieces = [halves(w.astype(BF), 1) for w in (query_weight, key_weight, value_weight, gate_weight)]
    mine = jnp.concatenate([p[0] for p in pieces], axis=1)
    other = jnp.concatenate([p[1] for p in pieces], axis=1)
    w_heads = place(collect(mine, other), "fs")

    owned = (query_scale, key_scale, value_scale, gate_scale, out_scale, up_scale, down_scale)
    packed = jnp.concatenate(owned)[None, :]
    packed = place(spread({0: packed}, "fs", fs_bits), "fs")
    scales, start = [], 0
    for scale in owned:
        scales.append(packed[:, start : start + scale.shape[0]].reshape(-1))
        start += scale.shape[0]
    o_scale, u_scale, d_scale = scales[4:]
    head_scale = jnp.concatenate([halves(s, 0)[0] for s in scales[:4]])

    w_out = place(spread({0: out_weight.astype(BF).T}, "fs", fs_bits), "fs")
    w_up = place(collect(*halves(up_weight.astype(BF), 1)), "fs")
    w_down = place(collect(*halves(down_weight.astype(BF).T, 1)), "fs")

    normed = norm_columns(whole, mix_gain)
    projected = (contract_first(normed, w_heads) * head_scale[None, :]).astype(BF)
    heads = forget.shape[0] // 2
    group = query_weight.shape[1] // 2
    shape = (2, length, heads, group // heads)
    query, key, value, gate = (
        projected[:, n * group : (n + 1) * group].reshape(shape) for n in range(4)
    )
    mixed = retain(query, key, value, gate, halves(forget, 0)[0]).astype(BF)
    mixed = mixed.reshape(2, length, group)
    theirs = swap(mixed[1], "fs", PAIR)
    mixed = jnp.where(
        side == 0,
        jnp.concatenate([mixed[0], theirs], axis=1),
        jnp.concatenate([theirs, mixed[0]], axis=1),
    )
    part = lax.dot_general(w_out, mixed, (((1,), (1,)), ((), ())), preferred_element_type=F32)
    mix_total = reduce_tp(part.astype(BF))
    after_mix = (tokens.astype(F32) + mix_total * o_scale[:, None]).astype(BF)

    normed_mlp = norm_columns(gather_tokens(after_mix), mlp_gain)
    upper = contract_first(w_up, normed_mlp) * halves(u_scale, 0)[0][:, None]
    hidden = jnp.square(jax.nn.relu(upper)).astype(BF)
    part = jnp.dot(w_down, hidden, preferred_element_type=F32).astype(BF)
    theirs = reduce_tp(part[:, length:])
    mine = reduce_tp(part[:, :length])
    mlp_total = mine + swap(theirs.astype(BF), "fs", PAIR).astype(F32)
    return (after_mix.astype(F32) + mlp_total * d_scale[:, None]).astype(BF)


def solution(mesh):
    in_specs = (
        P("tp", "fs"),
        P(),
        P(),
        P("fs", "tp"),
        P("fs", "tp"),
        P("fs", "tp"),
        P("fs", "tp"),
        P("tp", "fs"),
        P("fs", "tp"),
        P("tp", "fs"),
        P(("tp", "fs")),
        P(("tp", "fs")),
        P(("tp", "fs")),
        P(("tp", "fs")),
        P(("tp", "fs")),
        P(("tp", "fs")),
        P(("tp", "fs")),
        P("tp"),
    )
    out_specs = P("tp", "fs")
    return jax.shard_map(
        on_device, mesh=mesh, in_specs=in_specs, out_specs=out_specs, check_vma=False
    )
```
